512 devices in a mesh: ep: 128 (over z, x, core), tp: 4 (over y).
Axes of the slice: x: 4, y: 4, z: 16, core: 2. Of those that a mesh axis runs over, the one named last changes fastest.
Arguments:
- tokens: bfloat16 [16384, 2048], P('ep', 'tp'), may hold values from -6 to 6
- cotangent: bfloat16 [16384, 2048], P('ep', 'tp'), may hold values from -6 to 6
- experts: int32 [16384, 2], P('ep'), may hold values from 0 to 127, as said below
- combine: float32 [16384, 2], P('ep'), may hold values from 0.2 to 1
- w_gate: bfloat16 [128, 2048, 256], P('ep', 'tp'), may hold values from -0.125 to 0.125
- w_up: bfloat16 [128, 2048, 256], P('ep', 'tp'), may hold values from -0.125 to 0.125
- w_down: bfloat16 [128, 256, 2048], P('ep', None, 'tp'), may hold values from -0.375 to 0.375
Outputs:
- grad_tokens: bfloat16 [16384, 2048], P('ep', 'tp')
- grad_combine: float32 [16384, 2], P('ep')
- gate_grad: float32 [128, 2048, 256], P('ep', 'tp')
- up_grad: float32 [128, 2048, 256], P('ep', 'tp')
- down_grad: float32 [128, 256, 2048], P('ep', None, 'tp')
The draws below stay inside these ranges and needn't reach their ends.
Inputs may be any that keep to these rules, and one draw needn't show every extreme that they name: Each row names two different experts of one group of 4 consecutive experts. The rows of one index of ep name any one expert at most 4 times, and some expert exactly 4 times.
All inputs are finite; a program needn't handle non-finite values.
Results may differ from the reference program's by a relative error of at most 0.019.
Values may be sent and summed in bfloat16 or wider, within the bound.
No kernel may reach another device: no remote copies, remote signals or barrier semaphores. Data moves between devices by JAX's collectives and lax.ppermute only.
A program may use at most 64 MiB of HBM per device.

```python
import jax
import jax.numpy as jnp
from jax import lax

D = 2048
FE = 256
TOPK = 2
GSIZE = 4
TOK_DEV = 128
TOKENS = 16384
EXPERTS = 128
GROUPS = 32
CAP = 4
N_EP = 128
N_TP = 4


def draw_experts(key, part):
    base_group = jax.random.randint(jax.random.fold_in(key, 7), (), 0, GROUPS).astype(jnp.int32)
    device_keys = jax.random.split(jax.random.fold_in(key, 11), N_EP)
    device_ids = jnp.arange(N_EP, dtype=jnp.int32)

    def one_device(device_key, device_id):
        keys_four = jax.random.split(device_key, 4)
        hot_group = ((base_group + device_id) % GROUPS).astype(jnp.int32)
        pair_count = GROUPS // 2
        step_range = CAP // 4
        shifts = 4 * jax.random.randint(keys_four[0], (pair_count,), -step_range, step_range + 1).astype(jnp.int32)
        shifts = shifts.at[0].set(CAP)
        quotas = jnp.stack([CAP + shifts, CAP - shifts], axis=1).reshape(GROUPS).astype(jnp.int32)
        others = (hot_group + 1 + jnp.arange(GROUPS - 1, dtype=jnp.int32)) % GROUPS
        placed = jnp.concatenate([hot_group[None], jax.random.permutation(keys_four[1], others).astype(jnp.int32)])
        bounds = jnp.cumsum(quotas).astype(jnp.int32)
        ranks = jnp.arange(TOK_DEV, dtype=jnp.int32)
        position = jnp.searchsorted(bounds, ranks, side='right').astype(jnp.int32)
        within = ranks - (bounds[position] - quotas[position])
        inner_keys = jax.random.split(keys_four[2], GROUPS)
        inner_order = jax.vmap(lambda inner_key: jax.random.permutation(inner_key, GSIZE))(inner_keys).astype(jnp.int32)
        first_pick = inner_order[position, within % GSIZE]
        second_pick = inner_order[position, (within + 1) % GSIZE]
        expert_ids = placed[position][:, None] * GSIZE + jnp.stack([first_pick, second_pick], axis=1)
        order = jax.random.permutation(keys_four[3], TOK_DEV)
        return expert_ids[order].astype(jnp.int32)
    return jax.vmap(one_device)(device_keys, device_ids).reshape(TOKENS, TOPK)


def shard_levels(stream_key, extent, shards, least, top_value):
    def one(dim, parts):
        heights = jax.random.uniform(jax.random.fold_in(jax.random.fold_in(stream_key, 6), dim), (parts,), jnp.float32, least / len(shards), top_value / len(shards))
        return jnp.repeat(jnp.exp(heights), extent[dim] // parts).reshape((-1,) + (1,) * (len(extent) - dim - 1))

    factor_of = one(*shards[0])
    for cut in shards[1:]:
        factor_of = factor_of * one(*cut)
    return factor_of


def normal_values(stream_key, extent, deviation, bound, shards=(), held_as=jnp.bfloat16):
    gain = shard_levels(stream_key, extent, shards, -0.22, 0.18) if shards else 1.0
    result = jax.random.normal(stream_key, extent, jnp.float32) * deviation * gain
    return jnp.minimum(jnp.maximum(result, -bound), bound).astype(held_as)


def setup_inputs(seed: int = 0) -> dict:
    key_list = jax.random.split(jax.random.key(seed), 8)
    tokens = normal_values(key_list[0], (TOKENS, D), 1.0, 6.0, ((0, 128), (1, 4)))
    cotangent = normal_values(key_list[1], (TOKENS, D), 1.0, 6.0, ((0, 128), (1, 4)))
    experts = draw_experts(jax.random.fold_in(key_list[7], 71), 0)
    combine = jnp.clip(0.2 + 0.8 * jax.random.uniform(key_list[3], (TOKENS, TOPK), jnp.float32) ** shard_levels(key_list[3], (TOKENS, TOPK), ((0, 128),), -0.2, 0.2), 0.2, 1.0)
    w_gate = normal_values(key_list[4], (EXPERTS, D, FE), D ** -0.5, 0.125, ((0, 128), (1, 4)))
    w_up = normal_values(key_list[5], (EXPERTS, D, FE), D ** -0.5, 0.125, ((0, 128), (1, 4)))
    w_down = normal_values(key_list[6], (EXPERTS, FE, D), FE ** -0.5, 0.375, ((0, 128), (2, 4)))
    return dict(tokens=tokens, cotangent=cotangent, experts=experts, combine=combine, w_gate=w_gate, w_up=w_up, w_down=w_down)


def slot_table(experts):
    routed = experts.reshape(N_EP, TOK_DEV * TOPK).astype(jnp.int32)
    onehot = (routed[:, :, None] == jnp.arange(EXPERTS, dtype=jnp.int32)[None, None, :]).astype(jnp.int32)
    earlier = jnp.sum((jnp.cumsum(onehot, axis=1) - onehot) * onehot, axis=2).astype(jnp.int32)
    position = jnp.arange(N_EP, dtype=jnp.int32)[:, None] * CAP + earlier
    assigned = jnp.arange(TOKENS * TOPK, dtype=jnp.int32).reshape(N_EP, TOK_DEV * TOPK)
    table = jnp.full((EXPERTS, N_EP * CAP), -1, jnp.int32)
    return table.at[routed, position].set(assigned)


def block_sum(partial_sum):
    rounded = lax.optimization_barrier(partial_sum.astype(jnp.bfloat16)).astype(jnp.float32)
    return jnp.sum(rounded, axis=1)


def reference(tokens, cotangent, experts, combine, w_gate, w_up, w_down):
    table = slot_table(experts)
    weight_flat = lax.optimization_barrier(combine.astype(jnp.bfloat16)).astype(jnp.float32).reshape(-1)
    width_block = D // N_TP
    highest = lax.Precision.HIGHEST

    def per_expert(running, inputs):
        grad_acc, comb_acc = running
        row_ids, gate_mat, up_mat, down_mat = inputs
        filled = row_ids >= 0
        source = jnp.maximum(row_ids, 0)
        token_ids = (source // TOPK).astype(jnp.int32)
        filled_col = filled[:, None]
        rows = jnp.where(filled_col, tokens[token_ids], jnp.zeros((), jnp.bfloat16))
        cots = jnp.where(filled_col, cotangent[token_ids], jnp.zeros((), jnp.bfloat16))
        weights = jnp.where(filled, weight_flat[source], jnp.float32(0.0))[:, None]
        rows_split = rows.astype(jnp.float32).reshape(-1, N_TP, width_block)
        cots_split = cots.astype(jnp.float32).reshape(-1, N_TP, width_block)
        gate_blocks = gate_mat.astype(jnp.float32).reshape(N_TP, width_block, FE)
        up_blocks = up_mat.astype(jnp.float32).reshape(N_TP, width_block, FE)
        down_blocks = down_mat.astype(jnp.float32).reshape(FE, N_TP, width_block)
        gate_pre = block_sum(jnp.einsum('rjd,jdf->rjf', rows_split, gate_blocks, precision=highest))
        up_pre = block_sum(jnp.einsum('rjd,jdf->rjf', rows_split, up_blocks, precision=highest))
        grad_scaled = block_sum(jnp.einsum('rjd,fjd->rjf', cots_split, down_blocks, precision=highest))
        sigmoid_val = jax.nn.sigmoid(gate_pre)
        silu_val = gate_pre * sigmoid_val
        hidden = silu_val * up_pre
        scaled = (weights * hidden).astype(jnp.bfloat16)
        comb_part = jnp.sum(hidden * grad_scaled, axis=1)
        grad_hidden = weights * grad_scaled
        grad_gate_pre = (grad_hidden * up_pre * sigmoid_val * (1.0 + gate_pre * (1.0 - sigmoid_val))).astype(jnp.bfloat16)
        grad_up_pre = (grad_hidden * silu_val).astype(jnp.bfloat16)
        down_grad = jnp.dot(scaled.T, cots, preferred_element_type=jnp.float32)
        gate_grad = jnp.dot(rows.T, grad_gate_pre, preferred_element_type=jnp.float32)
        up_grad = jnp.dot(rows.T, grad_up_pre, preferred_element_type=jnp.float32)
        slot_grad = (jnp.dot(grad_gate_pre, gate_mat.T, preferred_element_type=jnp.float32) + jnp.dot(grad_up_pre, up_mat.T, preferred_element_type=jnp.float32)).astype(jnp.bfloat16)
        grad_acc = grad_acc.at[token_ids].add(jnp.where(filled_col, slot_grad.astype(jnp.float32), jnp.float32(0.0)))
        comb_acc = comb_acc.at[source].add(jnp.where(filled, comb_part, jnp.float32(0.0)))
        return (grad_acc, comb_acc), (gate_grad, up_grad, down_grad)

    start_carry = (jnp.zeros((TOKENS, D), jnp.float32), jnp.zeros((TOKENS * TOPK,), jnp.float32))
    (grad_acc, comb_acc), (gate_grad, up_grad, down_grad) = lax.scan(per_expert, start_carry, (table, w_gate, w_up, w_down))
    return grad_acc.astype(jnp.bfloat16), comb_acc.reshape(TOKENS, TOPK), gate_grad, up_grad, down_grad
```

```python
import jax
import jax.numpy as jnp
from jax import lax
from jax.sharding import PartitionSpec as P

BF = jnp.bfloat16
F32 = jnp.float32
GROUP = 4
CAP = 8
LANES = 128


def exchange_groups(peers):
    planes = peers // 8
    groups = []
    for low in (0, 1):
        for core in (0, 1):
            groups.append([z * 8 + x * 2 + core for z in range(planes) for x in (low, 3 - low)])
    return groups


def partner(peers, bit):
    return [(i, i ^ bit) for i in range(peers)]


def dot(a, b, contract):
    return lax.dot_general(a, b, (contract, ((), ())), preferred_element_type=F32)


def split_hi_lo(v):
    hi = v.astype(BF)
    return hi, (v - hi.astype(F32)).astype(BF)


def body(tokens, cotangent, experts, combine, w_gate, w_up, w_down):
    peers = lax.axis_size("ep")
    widths = lax.axis_size("tp")
    tok_count, block = tokens.shape
    hidden = w_gate.shape[2]
    n_groups = peers // GROUP
    slots = n_groups * CAP
    share = slots // widths
    groups = exchange_groups(peers)
    mine = lax.axis_index("ep") % GROUP

    gu = jnp.concatenate([w_gate[0], w_up[0]], axis=0)
    gu_x = lax.ppermute(gu, "ep", partner(peers, 2))
    wd_x = lax.ppermute(w_down[0], "ep", partner(peers, 2))
    gu2 = jnp.stack([gu, gu_x])
    wd2 = jnp.stack([w_down[0], wd_x])
    gu4 = jnp.concatenate([gu2, lax.ppermute(gu2, "ep", partner(peers, 1))])
    wd4 = jnp.concatenate([wd2, lax.ppermute(wd2, "ep", partner(peers, 1))])
    order = (0, 2, 1, 3)
    wg4, wu4 = gu4[:, :block], gu4[:, block:]

    group = experts[:, 0] // GROUP
    same = (group[:, None] == group[None, :]) & (
        jnp.arange(tok_count)[None, :] < jnp.arange(tok_count)[:, None]
    )
    slot = group * CAP + jnp.sum(same.astype(jnp.int32), axis=1)
    place = (jnp.arange(slots)[:, None] == slot[None, :]).astype(BF)
    local = experts % GROUP
    weight_b = combine.astype(BF)
    lane = jnp.arange(LANES)[None, :]
    meta = jnp.where(lane == local[:, :1], weight_b[:, :1], 0) + jnp.where(
        lane == local[:, 1:], weight_b[:, 1:], 0
    )
    rows_out = jnp.concatenate([tokens, cotangent, meta.astype(BF)], axis=1)
    payload = dot(place, rows_out, ((1,), (0,))).astype(BF).reshape(n_groups, CAP, -1)
    arrived = lax.all_to_all(
        payload, "ep", split_axis=0, concat_axis=0, tiled=True, axis_index_groups=groups
    ).reshape(slots, -1)
    rows = arrived[:, :block]
    cots = arrived[:, block : 2 * block]
    w4 = arrived[:, 2 * block : 2 * block + GROUP].astype(F32)
    used = w4 > 0
    before = jnp.cumsum(used.astype(jnp.int32), axis=1) - used
    picks_abs = [used & (before == k) for k in (0, 1)]
    picks = [
        [jnp.any(p & (jnp.arange(GROUP)[None, :] == (mine ^ r)), axis=1, keepdims=True) for r in order]
        for p in picks_abs
    ]

    def picked(dense):
        out = []
        for k in (0, 1):
            acc = jnp.zeros(dense[0].shape, F32)
            for r in range(GROUP):
                acc = jnp.where(picks[k][r], dense[r], acc)
            out.append(acc.astype(BF))
        return out

    gate = picked([dot(rows, wg4[r], ((1,), (0,))) for r in range(GROUP)])
    up = picked([dot(rows, wu4[r], ((1,), (0,))) for r in range(GROUP)])
    down = picked([dot(cots, wd4[r], ((1,), (1,))) for r in range(GROUP)])
    parts = jnp.concatenate(
        [gate[0], up[0], down[0], gate[1], up[1], down[1]], axis=1
    ).reshape(widths, share, 6 * hidden)
    sums = (
        lax.all_to_all(parts, "tp", split_axis=0, concat_axis=0, tiled=True)
        .astype(F32)
        .sum(axis=0)
    )
    w_pick = [jnp.sum(jnp.where(p, w4, 0.0), axis=1, keepdims=True) for p in picks_abs]
    me = lax.axis_index("tp")
    sent, combs = [], []
    for k in (0, 1):
        w = lax.dynamic_slice_in_dim(w_pick[k], me * share, share, 0)
        gate_pre, up_pre, grad_scaled = (
            sums[:, (3 * k + i) * hidden : (3 * k + i + 1) * hidden] for i in range(3)
        )
        sig = jax.nn.sigmoid(gate_pre)
        silu = gate_pre * sig
        hid = silu * up_pre
        gh = w * grad_scaled
        sent.append((w * hid).astype(BF))
        sent.append((gh * up_pre * sig * (1.0 + gate_pre * (1.0 - sig))).astype(BF))
        sent.append((gh * silu).astype(BF))
        combs.extend(split_hi_lo(jnp.sum(hid * grad_scaled, axis=1, keepdims=True)))
    pad = jnp.zeros((share, LANES - 4), BF)
    acts = lax.all_gather(
        jnp.concatenate(sent + combs + [pad], axis=1), "tp", axis=0, tiled=True
    )

    def spread(i):
        a = [acts[:, (3 * k + i) * hidden : (3 * k + i + 1) * hidden] for k in (0, 1)]
        zero = jnp.zeros((), BF)
        return [
            jnp.where(picks[0][r], a[0], jnp.where(picks[1][r], a[1], zero)) for r in range(GROUP)
        ]

    scaled4, ggp4, gup4 = spread(0), spread(1), spread(2)
    slot_sum = sum(
        dot(ggp4[r], wg4[r], ((1,), (1,))) + dot(gup4[r], wu4[r], ((1,), (1,)))
        for r in range(GROUP)
    )
    back = jnp.concatenate(
        [slot_sum.astype(BF), acts[:, 6 * hidden : 6 * hidden + LANES]], axis=1
    ).reshape(n_groups, CAP, -1)
    returned = lax.all_to_all(
        back, "ep", split_axis=0, concat_axis=0, tiled=True, axis_index_groups=groups
    ).reshape(slots, -1)

    def partials(r):
        return (
            dot(rows, ggp4[r], ((0,), (0,))),
            dot(rows, gup4[r], ((0,), (0,))),
            dot(scaled4[r], cots, ((0,), (0,))),
        )

    part = [partials(r) for r in range(GROUP)]
    sib_gu = jnp.stack([jnp.concatenate(part[r][:2]).astype(BF) for r in (2, 3)])
    sib_d = jnp.stack([part[r][2].astype(BF) for r in (2, 3)])
    got_gu = lax.ppermute(sib_gu, "ep", partner(peers, 1)).astype(F32)
    got_d = lax.ppermute(sib_d, "ep", partner(peers, 1)).astype(F32)
    half_gu = [jnp.concatenate(part[r][:2]) + got_gu[r] for r in (0, 1)]
    half_d = [part[r][2] + got_d[r] for r in (0, 1)]
    total_gu = half_gu[0] + lax.ppermute(half_gu[1].astype(BF), "ep", partner(peers, 2)).astype(F32)
    total_d = half_d[0] + lax.ppermute(half_d[1].astype(BF), "ep", partner(peers, 2)).astype(F32)

    found = dot(place, returned, ((0,), (0,)))
    grad_tokens = found[:, :block].astype(BF)
    comb = [found[:, block + 2 * k : block + 2 * k + 1] + found[:, block + 2 * k + 1 : block + 2 * k + 2] for k in (0, 1)]
    first = local[:, :1] < local[:, 1:]
    grad_combine = jnp.concatenate(
        [jnp.where(first, comb[0], comb[1]), jnp.where(first, comb[1], comb[0])], axis=1
    )
    return (grad_tokens, grad_combine, total_gu[None, :block], total_gu[None, block:], total_d[None])


def solution(mesh):
    return jax.shard_map(
        body,
        mesh=mesh,
        in_specs=(
            P("ep", "tp"),
            P("ep", "tp"),
            P("ep", None),
            P("ep", None),
            P("ep", "tp", None),
            P("ep", "tp", None),
            P("ep", None, "tp"),
        ),
        out_specs=(
            P("ep", "tp"),
            P("ep", None),
            P("ep", "tp", None),
            P("ep", "tp", None),
            P("ep", None, "tp"),
        ),
        check_vma=False,
    )
```

```python
import jax
import jax.numpy as jnp
from jax import lax
from jax.experimental import pallas as pl
from jax.experimental.pallas import tpu as pltpu
from jax.sharding import PartitionSpec as P

BF = jnp.bfloat16
F32 = jnp.float32
I32 = jnp.int32
GROUP = 4
CAP = 8
LANES = 128
ORDER = (0, 2, 1, 3)


def exchange_groups(peers):
    planes = peers // 8
    groups = []
    for low in (0, 1):
        for core in (0, 1):
            groups.append([z * 8 + x * 2 + core for x in (low, 3 - low) for z in range(planes)])
    return groups


def partner(peers, bit):
    return [(i, i ^ bit) for i in range(peers)]


def dot(a, b, ca, cb):
    return lax.dot_general(a, b, (((ca,), (cb,)), ((), ())), preferred_element_type=F32)


def iota(shape, dim):
    return lax.broadcasted_iota(I32, shape, dim)


def call(kernel, outs, *args, **kwargs):
    return pl.pallas_call(
        kernel,
        out_shape=outs,
        compiler_params=pltpu.CompilerParams(vmem_limit_bytes=20 * 1024 * 1024),
        **kwargs,
    )(*args)


def shape(dims, dtype):
    return jax.ShapeDtypeStruct(dims, dtype)


def placement(experts, n_groups):
    toks = experts.shape[1]
    group = lax.shift_right_logical(experts[0:1, :], 2)
    group = (group & 1) * (n_groups // 2) + lax.shift_right_logical(group, 1)
    member = iota((n_groups, toks), 0) == group
    onehot = jnp.where(member, 1.0, 0.0)
    earlier = jnp.where(iota((toks, toks), 0) < iota((toks, toks), 1), 1.0, 0.0).astype(BF)
    cum = dot(onehot.astype(BF), earlier, 1, 0)
    pos = jnp.sum(onehot * cum, axis=0, keepdims=True).astype(I32)
    slot = group * CAP + pos
    return jnp.where(iota((n_groups * CAP, toks), 0) == slot, 1.0, 0.0).astype(BF)


def send_kernel(tok_hbm, cot_hbm, exp_hbm, comb_hbm, out_ref, tok_ref, cot_ref, exp_ref, comb_ref, sems):
    copies = [
        pltpu.make_async_copy(src, dst, sems.at[i])
        for i, (src, dst) in enumerate(
            ((exp_hbm, exp_ref), (comb_hbm, comb_ref), (tok_hbm, tok_ref), (cot_hbm, cot_ref))
        )
    ]
    for copy in copies:
        copy.start()
    for copy in copies:
        copy.wait()
    block = tok_ref.shape[1]
    toks = tok_ref.shape[0]
    n_groups = out_ref.shape[0] // CAP
    experts = exp_ref[...]
    place = placement(experts, n_groups)
    local = experts & (GROUP - 1)
    weight = comb_ref[...].astype(BF).astype(F32)
    row = iota((LANES, toks), 0)
    meta = jnp.where(row == local[0:1, :], weight[0:1, :], 0.0) + jnp.where(
        row == local[1:2, :], weight[1:2, :], 0.0
    )
    out_ref[:, :block] = dot(place, tok_ref[...], 1, 0).astype(BF)
    out_ref[:, block : 2 * block] = dot(place, cot_ref[...], 1, 0).astype(BF)
    out_ref[:, 2 * block :] = dot(place, meta.astype(BF), 1, 1).astype(BF)


def chosen(meta):
    lane = iota(meta.shape, 1)
    used = meta > 0
    first = jnp.min(jnp.where(used, lane, 99), axis=1, keepdims=True)
    second = jnp.max(jnp.where(used, lane, -1), axis=1, keepdims=True)
    return first, second


def picks(meta, hidden):
    first, second = chosen(meta)
    wide = (meta.shape[0], hidden)
    return jnp.broadcast_to(first, wide), jnp.broadcast_to(second, wide)


def weights(w_refs, r, rows):
    return w_refs[r][rows, :]


def parts_kernel(arr_ref, own_ref, sib_ref, x_ref, xsib_ref, out_ref):
    w_refs = (own_ref, sib_ref, x_ref, xsib_ref)
    hidden = own_ref.shape[1]
    block = own_ref.shape[0] // 6 * 2
    mine = lax.axis_index("ep") & (GROUP - 1)
    first, second = picks(arr_ref[:, 2 * block :].astype(F32), hidden)
    rows = arr_ref[:, :block]
    for q in range(3):
        p0 = jnp.zeros(first.shape, F32)
        p1 = p0
        for r in ORDER:
            if q < 2:
                dense = dot(rows, weights(w_refs, r, slice(q * block, (q + 1) * block)), 1, 0)
            else:
                half = block // 2
                dense = dot(
                    arr_ref[:, block : block + half],
                    weights(w_refs, r, slice(2 * block, 2 * block + half)),
                    1,
                    1,
                ) + dot(
                    arr_ref[:, block + half : 2 * block],
                    weights(w_refs, r, slice(2 * block + half, 3 * block)),
                    1,
                    1,
                )
            expert = mine ^ r
            p0 = jnp.where(first == expert, dense, p0)
            p1 = jnp.where(second == expert, dense, p1)
        out_ref[:, q * hidden : (q + 1) * hidden] = p0.astype(BF)
        out_ref[:, (3 + q) * hidden : (4 + q) * hidden] = p1.astype(BF)


def act_kernel(part_ref, arr_ref, out_ref):
    share = part_ref.shape[1]
    hidden = part_ref.shape[2] // 6
    meta_at = arr_ref.shape[1] - LANES
    me = lax.axis_index("tp")
    meta = arr_ref[pl.ds(pl.multiple_of(me * share, share), share), meta_at:].astype(F32)
    first, second = chosen(meta)
    lane = iota((share, LANES), 1)
    extra = jnp.zeros((share, LANES), F32)
    for k, pick in enumerate((first, second)):
        weight = jnp.sum(jnp.where(lane == pick, meta, 0.0), axis=1, keepdims=True)
        total = []
        for q in range(3):
            at = slice((3 * k + q) * hidden, (3 * k + q + 1) * hidden)
            acc = part_ref[0, :, at].astype(F32)
            for d in range(1, part_ref.shape[0]):
                acc = acc + part_ref[d, :, at].astype(F32)
            total.append(acc)
        gate_pre, up_pre, grad_scaled = total
        sig = jax.nn.sigmoid(gate_pre)
        silu = gate_pre * sig
        hid = silu * up_pre
        gh = weight * grad_scaled
        at = 3 * k * hidden
        out_ref[:, at : at + hidden] = (weight * hid).astype(BF)
        out_ref[:, at + hidden : at + 2 * hidden] = (
            gh * up_pre * sig * (1.0 + gate_pre * (1.0 - sig))
        ).astype(BF)
        out_ref[:, at + 2 * hidden : at + 3 * hidden] = (gh * silu).astype(BF)
        comb = jnp.sum(hid * grad_scaled, axis=1, keepdims=True)
        high = comb.astype(BF).astype(F32)
        extra = jnp.where(lane == 2 * k, high, jnp.where(lane == 2 * k + 1, comb - high, extra))
    out_ref[:, 6 * hidden :] = extra.astype(BF)


def masks(arr_ref, hidden):
    mine = lax.axis_index("ep") & (GROUP - 1)
    meta = arr_ref[:, arr_ref.shape[1] - LANES :].astype(F32)
    first, second = picks(meta, hidden)
    out = {}
    for r in ORDER:
        expert = mine ^ r
        out[r] = tuple(jnp.where(p == expert, 1.0, 0.0).astype(BF) for p in (first, second))
    return out


def spread(act_ref, mask, q, hidden):
    return (
        act_ref[:, q * hidden : (q + 1) * hidden] * mask[0]
        + act_ref[:, (3 + q) * hidden : (4 + q) * hidden] * mask[1]
    )


def back_kernel(act_ref, arr_ref, own_ref, sib_ref, x_ref, xsib_ref, out_ref):
    w_refs = (own_ref, sib_ref, x_ref, xsib_ref)
    hidden = own_ref.shape[1]
    block = own_ref.shape[0] // 6 * 2
    mask = masks(arr_ref, hidden)
    acc = jnp.zeros((act_ref.shape[0], block), F32)
    for r in ORDER:
        for q in (1, 2):
            w = weights(w_refs, r, slice((q - 1) * block, q * block))
            acc = acc + dot(spread(act_ref, mask[r], q, hidden), w, 1, 1)
    out_ref[:, :block] = acc.astype(BF)
    out_ref[:, block:] = act_ref[:, 6 * hidden :]


def stacked(block):
    half = block // 2
    return (
        slice(0, block),
        slice(block, 2 * block),
        slice(2 * block, 2 * block + half),
        slice(2 * block + half, 3 * block),
    )


def grads_kernel(act_ref, arr_ref, send_ref, pass_ref, keep_ref):
    hidden = send_ref.shape[2]
    block = send_ref.shape[1] // 3
    g, u, d0, d1 = stacked(block)
    mask = masks(arr_ref, hidden)
    rows = arr_ref[:, :block]
    cots = arr_ref[:, block : 2 * block]
    for r, ref in ((1, send_ref.at[0]), (3, send_ref.at[1]), (2, pass_ref), (0, keep_ref)):
        ref[g, :] = dot(rows, spread(act_ref, mask[r], 1, hidden), 0, 0).astype(BF)
        ref[u, :] = dot(rows, spread(act_ref, mask[r], 2, hidden), 0, 0).astype(BF)
        down = dot(spread(act_ref, mask[r], 0, hidden), cots, 0, 0).astype(BF)
        ref[d0, :] = down[:, : block // 2]
        ref[d1, :] = down[:, block // 2 :]


def half_kernel(pass_ref, got_ref, out_ref):
    out_ref[...] = (pass_ref[...].astype(F32) + got_ref[1].astype(F32)).astype(BF)


def total_kernel(keep_ref, got_ref, last_ref, gate_ref, up_ref, down_ref):
    block = gate_ref.shape[0]
    g, u, d0, d1 = stacked(block)

    def total(at):
        return keep_ref[at, :].astype(F32) + got_ref[0, at, :].astype(F32) + last_ref[at, :].astype(F32)

    gate_ref[...] = total(g)
    up_ref[...] = total(u)
    down_ref[:, : block // 2] = total(d0)
    down_ref[:, block // 2 :] = total(d1)


def final_kernel(ret_ref, exp_ref, tok_ref, comb_ref):
    block = tok_ref.shape[1]
    experts = exp_ref[...]
    place = placement(experts, ret_ref.shape[0] // CAP)
    tok_ref[...] = dot(place, ret_ref[:, :block], 0, 0).astype(BF)
    extra = dot(ret_ref[:, block:], place, 0, 0)
    low = extra[0:1, :] + extra[1:2, :]
    high = extra[2:3, :] + extra[3:4, :]
    rising = experts[0:1, :] < experts[1:2, :]
    comb_ref[0:1, :] = jnp.where(rising, low, high)
    comb_ref[1:2, :] = jnp.where(rising, high, low)


def body(tokens, cotangent, experts, combine, w_gate, w_up, w_down):
    peers = lax.axis_size("ep")
    widths = lax.axis_size("tp")
    toks, block = tokens.shape
    hidden = w_gate.shape[2]
    n_groups = peers // GROUP
    slots = n_groups * CAP
    share = slots // widths
    groups = exchange_groups(peers)
    half = block // 2

    sources = (tokens, cotangent, experts.T, combine.T)
    payload = call(
        send_kernel,
        shape((slots, 2 * block + LANES), BF),
        *(pltpu.with_memory_space_constraint(a, pltpu.HBM) for a in sources),
        in_specs=[pl.BlockSpec(memory_space=pltpu.HBM)] * 4,
        scratch_shapes=[pltpu.VMEM(a.shape, a.dtype) for a in sources]
        + [pltpu.SemaphoreType.DMA((4,))],
    )
    arrived = lax.all_to_all(
        payload.reshape(n_groups, CAP, -1),
        "ep",
        split_axis=0,
        concat_axis=0,
        tiled=True,
        axis_index_groups=groups,
    ).reshape(slots, -1)
    arrived = pltpu.with_memory_space_constraint(arrived, pltpu.VMEM)
    own = jnp.concatenate([w_gate[0], w_up[0], w_down[0][:, :half], w_down[0][:, half:]], axis=0)
    other = lax.ppermute(own, "ep", partner(peers, 2))
    sibling = lax.ppermute(own, "ep", partner(peers, 1))
    across = lax.ppermute(other, "ep", partner(peers, 1))
    w_all = tuple(
        pltpu.with_memory_space_constraint(w, pltpu.VMEM) for w in (own, sibling, other, across)
    )
    parts = call(parts_kernel, shape((slots, 6 * hidden), BF), arrived, *w_all)
    pieces = lax.all_to_all(
        parts.reshape(widths, share, -1), "tp", split_axis=0, concat_axis=0, tiled=True
    )
    acts = call(act_kernel, shape((share, 6 * hidden + LANES), BF), pieces, arrived)
    acts = lax.all_gather(acts, "tp", axis=0, tiled=True)
    acts = pltpu.with_memory_space_constraint(acts, pltpu.VMEM)
    back = call(back_kernel, shape((slots, block + LANES), BF), acts, arrived, *w_all)
    returned = lax.all_to_all(
        back.reshape(n_groups, CAP, -1),
        "ep",
        split_axis=0,
        concat_axis=0,
        tiled=True,
        axis_index_groups=groups,
    ).reshape(slots, -1)
    stack = (3 * block, hidden)
    send, through, keep = call(
        grads_kernel, (shape((2, *stack), BF), shape(stack, BF), shape(stack, BF)), acts, arrived
    )
    got = lax.ppermute(send, "ep", partner(peers, 1))
    pair = call(half_kernel, shape(stack, BF), through, got)
    last = lax.ppermute(pair, "ep", partner(peers, 2))
    gate_grad, up_grad, down_grad = call(
        total_kernel,
        (shape((block, hidden), F32), shape((block, hidden), F32), shape((hidden, block), F32)),
        keep,
        got,
        last,
    )
    grad_tokens, comb = call(
        final_kernel, (shape((toks, block), BF), shape((2, toks), F32)), returned, experts.T
    )
    return (grad_tokens, comb.T, gate_grad[None], up_grad[None], down_grad[None])


def solution(mesh):
    return jax.shard_map(
        body,
        mesh=mesh,
        in_specs=(
            P("ep", "tp"),
            P("ep", "tp"),
            P("ep", None),
            P("ep", None),
            P("ep", "tp", None),
            P("ep", "tp", None),
            P("ep", None, "tp"),
        ),
        out_specs=(
            P("ep", "tp"),
            P("ep", None),
            P("ep", "tp", None),
            P("ep", "tp", None),
            P("ep", None, "tp"),
        ),
        check_vma=False,
    )
```

```python
import jax
import jax.numpy as jnp
from jax import lax
from jax.experimental import pallas as pl
from jax.experimental.pallas import tpu as pltpu
from jax.sharding import PartitionSpec as P

BF = jnp.bfloat16
F32 = jnp.float32
I32 = jnp.int32
GROUP = 4
CAP = 8
LANES = 128
ORDER = (0, 2, 1, 3)


def exchange_groups(peers):
    planes = peers // 8
    groups = []
    for low in (0, 1):
        for core in (0, 1):
            groups.append(
                [
                    z * 8 + x * 2 + core
                    for near in range(planes // 2)
                    for z in (near, near + planes // 2)
                    for x in (low, 3 - low)
                ]
            )
    return groups


def partner(peers, bit):
    return [(i, i ^ bit) for i in range(peers)]


def dot(a, b, ca, cb):
    return lax.dot_general(a, b, (((ca,), (cb,)), ((), ())), preferred_element_type=F32)


def iota(shape, dim):
    return lax.broadcasted_iota(I32, shape, dim)


def call(kernel, outs, *args, **kwargs):
    return pl.pallas_call(
        kernel,
        out_shape=outs,
        compiler_params=pltpu.CompilerParams(vmem_limit_bytes=20 * 1024 * 1024),
        **kwargs,
    )(*args)


def shape(dims, dtype):
    return jax.ShapeDtypeStruct(dims, dtype)


def placement(experts, n_groups):
    toks = experts.shape[1]
    group = lax.shift_right_logical(experts[0:1, :], 2)
    plane = lax.shift_right_logical(group, 1)
    planes = n_groups // 2
    plane = jnp.where(plane < planes // 2, 2 * plane, 2 * plane - planes + 1)
    group = 2 * plane + (group & 1)
    member = iota((n_groups, toks), 0) == group
    onehot = jnp.where(member, 1.0, 0.0)
    earlier = jnp.where(iota((toks, toks), 0) < iota((toks, toks), 1), 1.0, 0.0).astype(BF)
    cum = dot(onehot.astype(BF), earlier, 1, 0)
    pos = jnp.sum(onehot * cum, axis=0, keepdims=True).astype(I32)
    slot = group * CAP + pos
    return jnp.where(iota((n_groups * CAP, toks), 0) == slot, 1.0, 0.0).astype(BF)


def send_kernel(tok_hbm, cot_hbm, exp_hbm, comb_hbm, out_ref, tok_ref, cot_ref, exp_ref, comb_ref, sems):
    copies = [
        pltpu.make_async_copy(src, dst, sems.at[i])
        for i, (src, dst) in enumerate(
            ((exp_hbm, exp_ref), (comb_hbm, comb_ref), (tok_hbm, tok_ref), (cot_hbm, cot_ref))
        )
    ]
    for copy in copies:
        copy.start()
    for copy in copies:
        copy.wait()
    block = tok_ref.shape[1]
    toks = tok_ref.shape[0]
    n_groups = out_ref.shape[0] // CAP
    experts = exp_ref[...]
    place = placement(experts, n_groups)
    local = experts & (GROUP - 1)
    weight = comb_ref[...].astype(BF).astype(F32)
    row = iota((LANES, toks), 0)
    meta = jnp.where(row == local[0:1, :], weight[0:1, :], 0.0) + jnp.where(
        row == local[1:2, :], weight[1:2, :], 0.0
    )
    out_ref[:, :block] = dot(place, tok_ref[...], 1, 0).astype(BF)
    out_ref[:, block : 2 * block] = dot(place, cot_ref[...], 1, 0).astype(BF)
    out_ref[:, 2 * block :] = dot(place, meta.astype(BF), 1, 1).astype(BF)


def chosen(meta):
    lane = iota(meta.shape, 1)
    used = meta > 0
    first = jnp.min(jnp.where(used, lane, 99), axis=1, keepdims=True)
    second = jnp.max(jnp.where(used, lane, -1), axis=1, keepdims=True)
    return first, second


def picks(meta, hidden):
    first, second = chosen(meta)
    wide = (meta.shape[0], hidden)
    return jnp.broadcast_to(first, wide), jnp.broadcast_to(second, wide)


def parts_kernel(arr_ref, own_ref, sib_ref, x_ref, xsib_hbm, out_ref, xsib_ref, acc_ref, sem):
    fetch = pltpu.make_async_copy(xsib_hbm, xsib_ref, sem)
    fetch.start()
    w_refs = (own_ref, sib_ref, x_ref, xsib_ref)
    hidden = own_ref.shape[1]
    block = own_ref.shape[0] // 3
    half = block // 2
    mine = lax.axis_index("ep") & (GROUP - 1)
    first, second = picks(arr_ref[:, 2 * block :].astype(F32), hidden)

    def dense(q, r):
        if q < 2:
            return dot(arr_ref[:, :block], w_refs[r][q * block : (q + 1) * block, :], 1, 0)
        return dot(
            arr_ref[:, block : block + half], w_refs[r][2 * block : 2 * block + half, :], 1, 1
        ) + dot(arr_ref[:, block + half : 2 * block], w_refs[r][2 * block + half :, :], 1, 1)

    for q in range(3):
        p0 = jnp.zeros(first.shape, F32)
        p1 = p0
        for r in (0, 2, 1):
            part = dense(q, r)
            p0 = jnp.where(first == (mine ^ r), part, p0)
            p1 = jnp.where(second == (mine ^ r), part, p1)
        acc_ref[2 * q] = p0
        acc_ref[2 * q + 1] = p1
    fetch.wait()
    for q in range(3):
        part = dense(q, 3)
        p0 = jnp.where(first == (mine ^ 3), part, acc_ref[2 * q])
        p1 = jnp.where(second == (mine ^ 3), part, acc_ref[2 * q + 1])
        out_ref[:, q * hidden : (q + 1) * hidden] = p0.astype(BF)
        out_ref[:, (3 + q) * hidden : (4 + q) * hidden] = p1.astype(BF)


def act_kernel(part_ref, arr_ref, out_ref):
    share = part_ref.shape[1]
    hidden = part_ref.shape[2] // 6
    meta_at = arr_ref.shape[1] - LANES
    me = lax.axis_index("tp")
    meta = arr_ref[pl.ds(pl.multiple_of(me * share, share), share), meta_at:].astype(F32)
    first, second = chosen(meta)
    lane = iota((share, LANES), 1)
    extra = jnp.zeros((share, LANES), F32)
    for k, pick in enumerate((first, second)):
        weight = jnp.sum(jnp.where(lane == pick, meta, 0.0), axis=1, keepdims=True)
        total = []
        for q in range(3):
            at = slice((3 * k + q) * hidden, (3 * k + q + 1) * hidden)
            acc = part_ref[0, :, at].astype(F32)
            for d in range(1, part_ref.shape[0]):
                acc = acc + part_ref[d, :, at].astype(F32)
            total.append(acc)
        gate_pre, up_pre, grad_scaled = total
        sig = jax.nn.sigmoid(gate_pre)
        silu = gate_pre * sig
        hid = silu * up_pre
        gh = weight * grad_scaled
        at = 3 * k * hidden
        out_ref[:, at : at + hidden] = (weight * hid).astype(BF)
        out_ref[:, at + hidden : at + 2 * hidden] = (
            gh * up_pre * sig * (1.0 + gate_pre * (1.0 - sig))
        ).astype(BF)
        out_ref[:, at + 2 * hidden : at + 3 * hidden] = (gh * silu).astype(BF)
        comb = jnp.sum(hid * grad_scaled, axis=1, keepdims=True)
        high = comb.astype(BF).astype(F32)
        extra = jnp.where(lane == 2 * k, high, jnp.where(lane == 2 * k + 1, comb - high, extra))
    out_ref[:, 6 * hidden :] = extra.astype(BF)


def masks(arr_ref, hidden, experts=ORDER):
    mine = lax.axis_index("ep") & (GROUP - 1)
    meta = arr_ref[:, arr_ref.shape[1] - LANES :].astype(F32)
    first, second = picks(meta, hidden)
    out = {}
    for r in experts:
        expert = mine ^ r
        out[r] = tuple(jnp.where(p == expert, 1.0, 0.0).astype(BF) for p in (first, second))
    return out


def spread(act_ref, mask, q, hidden):
    return (
        act_ref[:, q * hidden : (q + 1) * hidden] * mask[0]
        + act_ref[:, (3 + q) * hidden : (4 + q) * hidden] * mask[1]
    )


def back_kernel(act_ref, arr_ref, own_ref, sib_ref, x_ref, xsib_hbm, out_ref, xsib_ref, sem):
    hidden = own_ref.shape[1]
    block = own_ref.shape[0] // 3
    fetch = pltpu.make_async_copy(xsib_hbm.at[: 2 * block, :], xsib_ref, sem)
    fetch.start()
    w_refs = (own_ref, sib_ref, x_ref, xsib_ref)
    mask = masks(arr_ref, hidden)
    acc = jnp.zeros((act_ref.shape[0], block), F32)
    for r in ORDER:
        if r == 3:
            fetch.wait()
        for q in (1, 2):
            w = w_refs[r][(q - 1) * block : q * block, :]
            acc = acc + dot(spread(act_ref, mask[r], q, hidden), w, 1, 1)
    out_ref[:, :block] = acc.astype(BF)
    out_ref[:, block:] = act_ref[:, 6 * hidden :]


def inner_parts(act_ref, arr_ref, mask, hidden):
    rows = arr_ref[:, : (arr_ref.shape[1] - LANES) // 2]
    return [dot(rows, spread(act_ref, mask, q, hidden), 0, 0) for q in (1, 2)]


def outer_part(act_ref, arr_ref, mask, hidden):
    block = (arr_ref.shape[1] - LANES) // 2
    return dot(spread(act_ref, mask, 0, hidden), arr_ref[:, block : 2 * block], 0, 0)


def inner_kernel(act_ref, arr_ref, send_ref, pass_ref):
    hidden = send_ref.shape[1]
    block = send_ref.shape[0] // 2
    mask = masks(arr_ref, hidden, (2, 3))
    for r, ref in ((3, send_ref), (2, pass_ref)):
        gate, up = inner_parts(act_ref, arr_ref, mask[r], hidden)
        ref[:block, :] = gate.astype(BF)
        ref[block:, :] = up.astype(BF)


def outer_kernel(act_ref, arr_ref, send_ref, pass_ref):
    hidden = send_ref.shape[0]
    mask = masks(arr_ref, hidden, (2, 3))
    for r, ref in ((3, send_ref), (2, pass_ref)):
        ref[...] = outer_part(act_ref, arr_ref, mask[r], hidden).astype(BF)


def half_kernel(pass_ref, got_ref, out_ref):
    out_ref[...] = (pass_ref[...].astype(F32) + got_ref[...].astype(F32)).astype(BF)


def sibling_kernel(act_ref, arr_ref, out_ref):
    hidden = out_ref.shape[1]
    block = out_ref.shape[0] // 3
    half = block // 2
    mask = masks(arr_ref, hidden, (1,))[1]
    gate, up = inner_parts(act_ref, arr_ref, mask, hidden)
    down = outer_part(act_ref, arr_ref, mask, hidden).astype(BF)
    out_ref[:block, :] = gate.astype(BF)
    out_ref[block : 2 * block, :] = up.astype(BF)
    out_ref[2 * block : 2 * block + half, :] = down[:, :half]
    out_ref[2 * block + half :, :] = down[:, half:]


def base_kernel(act_ref, arr_ref, got_ref, inner_ref, outer_ref):
    hidden = inner_ref.shape[1]
    block = inner_ref.shape[0] // 2
    half = block // 2
    mask = masks(arr_ref, hidden, (0,))[0]
    gate, up = inner_parts(act_ref, arr_ref, mask, hidden)
    down = outer_part(act_ref, arr_ref, mask, hidden)
    inner_ref[:block, :] = (gate + got_ref[:block, :].astype(F32)).astype(BF)
    inner_ref[block:, :] = (up + got_ref[block : 2 * block, :].astype(F32)).astype(BF)
    left = down[:, :half] + got_ref[2 * block : 2 * block + half, :].astype(F32)
    right = down[:, half:] + got_ref[2 * block + half :, :].astype(F32)
    outer_ref[:, :half] = left.astype(BF)
    outer_ref[:, half:] = right.astype(BF)


def total_kernel(base_ref, last_ref, *out_refs):
    rows = out_refs[0].shape[0]
    for i, out_ref in enumerate(out_refs):
        at = slice(i * rows, (i + 1) * rows)
        out_ref[...] = base_ref[at, :].astype(F32) + last_ref[at, :].astype(F32)


def final_kernel(ret_ref, exp_ref, tok_ref, comb_ref):
    block = tok_ref.shape[1]
    experts = exp_ref[...]
    place = placement(experts, ret_ref.shape[0] // CAP)
    tok_ref[...] = dot(place, ret_ref[:, :block], 0, 0).astype(BF)
    extra = dot(ret_ref[:, block:], place, 0, 0)
    low = extra[0:1, :] + extra[1:2, :]
    high = extra[2:3, :] + extra[3:4, :]
    rising = experts[0:1, :] < experts[1:2, :]
    comb_ref[0:1, :] = jnp.where(rising, low, high)
    comb_ref[1:2, :] = jnp.where(rising, high, low)


def body(tokens, cotangent, experts, combine, w_gate, w_up, w_down):
    peers = lax.axis_size("ep")
    widths = lax.axis_size("tp")
    toks, block = tokens.shape
    hidden = w_gate.shape[2]
    n_groups = peers // GROUP
    slots = n_groups * CAP
    share = slots // widths
    groups = exchange_groups(peers)
    half = block // 2

    sources = (tokens, cotangent, experts.T, combine.T)
    payload = call(
        send_kernel,
        shape((slots, 2 * block + LANES), BF),
        *(pltpu.with_memory_space_constraint(a, pltpu.HBM) for a in sources),
        in_specs=[pl.BlockSpec(memory_space=pltpu.HBM)] * 4,
        scratch_shapes=[pltpu.VMEM(a.shape, a.dtype) for a in sources]
        + [pltpu.SemaphoreType.DMA((4,))],
    )
    arrived = lax.all_to_all(
        payload.reshape(n_groups, CAP, -1),
        "ep",
        split_axis=0,
        concat_axis=0,
        tiled=True,
        axis_index_groups=groups,
    ).reshape(slots, -1)
    arrived = pltpu.with_memory_space_constraint(arrived, pltpu.VMEM)
    own = jnp.concatenate([w_gate[0], w_up[0], w_down[0][:, :half], w_down[0][:, half:]], axis=0)
    other = lax.ppermute(own, "ep", partner(peers, 2))
    sibling = lax.ppermute(own, "ep", partner(peers, 1))
    across = lax.ppermute(other, "ep", partner(peers, 1))
    w_all = tuple(
        pltpu.with_memory_space_constraint(w, space)
        for w, space in zip((own, sibling, other, across), (pltpu.VMEM,) * 3 + (pltpu.HBM,))
    )
    parts = call(
        parts_kernel,
        shape((slots, 6 * hidden), BF),
        arrived,
        *w_all,
        in_specs=[pl.BlockSpec(memory_space=pltpu.HBM if i == 4 else pltpu.VMEM) for i in range(5)],
        scratch_shapes=[
            pltpu.VMEM((3 * block, hidden), BF),
            pltpu.VMEM((6, slots, hidden), F32),
            pltpu.SemaphoreType.DMA,
        ],
    )
    pieces = lax.all_to_all(
        parts.reshape(widths, share, -1), "tp", split_axis=0, concat_axis=0, tiled=True
    )
    acts = call(act_kernel, shape((share, 6 * hidden + LANES), BF), pieces, arrived)
    acts = lax.all_gather(acts, "tp", axis=0, tiled=True)
    acts = pltpu.with_memory_space_constraint(acts, pltpu.VMEM)
    back = call(
        back_kernel,
        shape((slots, block + LANES), BF),
        acts,
        arrived,
        *w_all,
        in_specs=[pl.BlockSpec(memory_space=pltpu.HBM if i == 5 else pltpu.VMEM) for i in range(6)],
        scratch_shapes=[pltpu.VMEM((2 * block, hidden), BF), pltpu.SemaphoreType.DMA],
    )
    returned = lax.all_to_all(
        back.reshape(n_groups, CAP, -1),
        "ep",
        split_axis=0,
        concat_axis=0,
        tiled=True,
        axis_index_groups=groups,
    ).reshape(slots, -1)
    pairs = []
    for kernel, inputs, dims in (
        (inner_kernel, (acts, arrived), (2 * block, hidden)),
        (outer_kernel, (acts, arrived), (hidden, block)),
    ):
        send, through = call(kernel, (shape(dims, BF), shape(dims, BF)), *inputs)
        got = lax.ppermute(send, "ep", partner(peers, 1))
        pair = call(half_kernel, shape(dims, BF), through, got)
        pairs.append(lax.ppermute(pair, "ep", partner(peers, 2)))
    send = call(sibling_kernel, shape((3 * block, hidden), BF), acts, arrived)
    got = lax.ppermute(send, "ep", partner(peers, 1))
    base = call(
        base_kernel,
        (shape((2 * block, hidden), BF), shape((hidden, block), BF)),
        acts,
        arrived,
        got,
    )
    gate_grad, up_grad = call(total_kernel, (shape((block, hidden), F32),) * 2, base[0], pairs[0])
    (down_grad,) = call(total_kernel, (shape((hidden, block), F32),), base[1], pairs[1])
    grad_tokens, comb = call(
        final_kernel, (shape((toks, block), BF), shape((2, toks), F32)), returned, experts.T
    )
    return (grad_tokens, comb.T, gate_grad[None], up_grad[None], down_grad[None])


def solution(mesh):
    return jax.shard_map(
        body,
        mesh=mesh,
        in_specs=(
            P("ep", "tp"),
            P("ep", "tp"),
            P("ep", None),
            P("ep", None),
            P("ep", "tp", None),
            P("ep", "tp", None),
            P("ep", None, "tp"),
        ),
        out_specs=(
            P("ep", "tp"),
            P("ep", None),
            P("ep", "tp", None),
            P("ep", "tp", None),
            P("ep", None, "tp"),
        ),
        check_vma=False,
    )
```

```python
import jax
import jax.numpy as jnp
from jax import lax
from jax.experimental import pallas as pl
from jax.experimental.pallas import tpu as pltpu
from jax.sharding import PartitionSpec as P

BF = jnp.bfloat16
F32 = jnp.float32
I32 = jnp.int32
GROUP = 4
CAP = 8
LANES = 128
ORDER = (0, 2, 1, 3)


def exchange_groups(peers):
    planes = peers // 8
    groups = []
    for low in (0, 1):
        for core in (0, 1):
            groups.append(
                [
                    z * 8 + x * 2 + core
                    for near in range(planes // 4)
                    for z in (near + planes // 4 * q for q in (0, 2, 1, 3))
                    for x in (low, 3 - low)
                ]
            )
    return groups


def partner(peers, bit):
    return [(i, i ^ bit) for i in range(peers)]


def dot(a, b, ca, cb):
    return lax.dot_general(a, b, (((ca,), (cb,)), ((), ())), preferred_element_type=F32)


def iota(shape, dim):
    return lax.broadcasted_iota(I32, shape, dim)


def call(kernel, outs, *args, **kwargs):
    return pl.pallas_call(
        kernel,
        out_shape=outs,
        compiler_params=pltpu.CompilerParams(vmem_limit_bytes=20 * 1024 * 1024),
        **kwargs,
    )(*args)


def shape(dims, dtype):
    return jax.ShapeDtypeStruct(dims, dtype)


def placement(experts, n_groups):
    toks = experts.shape[1]
    group = lax.shift_right_logical(experts[0:1, :], 2)
    plane = lax.shift_right_logical(group, 1)
    planes = n_groups // 2
    quarter = plane // (planes // 4)
    middle = (quarter == 1) | (quarter == 2)
    plane = plane % (planes // 4) * 4 + jnp.where(middle, 3 - quarter, quarter)
    group = 2 * plane + (group & 1)
    member = iota((n_groups, toks), 0) == group
    onehot = jnp.where(member, 1.0, 0.0)
    earlier = jnp.where(iota((toks, toks), 0) < iota((toks, toks), 1), 1.0, 0.0).astype(BF)
    cum = dot(onehot.astype(BF), earlier, 1, 0)
    pos = jnp.sum(onehot * cum, axis=0, keepdims=True).astype(I32)
    slot = group * CAP + pos
    return jnp.where(iota((n_groups * CAP, toks), 0) == slot, 1.0, 0.0).astype(BF)


def send_kernel(
    tok_hbm, cot_hbm, exp_hbm, comb_hbm, out_hbm, tok_ref, cot_ref, exp_ref, comb_ref, out_ref, sems
):
    copies = [
        pltpu.make_async_copy(src, dst, sems.at[i])
        for i, (src, dst) in enumerate(
            ((exp_hbm, exp_ref), (tok_hbm, tok_ref), (cot_hbm, cot_ref), (comb_hbm, comb_ref))
        )
    ]
    for copy in copies:
        copy.start()
    toks, block = tok_ref.shape
    n_groups = out_ref.shape[0] // CAP
    copies[0].wait()
    experts = exp_ref[...]
    place = placement(experts, n_groups)
    local = experts & (GROUP - 1)
    row = iota((LANES, toks), 0)

    def written(first, last, i):
        copy = pltpu.make_async_copy(
            out_ref.at[:, first:last], out_hbm.at[:, first:last], sems.at[len(copies) + i]
        )
        copy.start()
        return copy

    copies[1].wait()
    out_ref[:, :block] = dot(place, tok_ref[...], 1, 0).astype(BF)
    rows_out = written(0, block, 0)
    copies[2].wait()
    copies[3].wait()
    weight = comb_ref[...].astype(BF).astype(F32)
    meta = jnp.where(row == local[0:1, :], weight[0:1, :], 0.0) + jnp.where(
        row == local[1:2, :], weight[1:2, :], 0.0
    )
    out_ref[:, block : 2 * block] = dot(place, cot_ref[...], 1, 0).astype(BF)
    out_ref[:, 2 * block :] = dot(place, meta.astype(BF), 1, 1).astype(BF)
    rest_out = written(block, 2 * block + LANES, 1)
    rows_out.wait()
    rest_out.wait()


def chosen(meta):
    lane = iota(meta.shape, 1)
    used = meta > 0
    first = jnp.min(jnp.where(used, lane, 99), axis=1, keepdims=True)
    second = jnp.max(jnp.where(used, lane, -1), axis=1, keepdims=True)
    return first, second


def picks(meta, hidden):
    first, second = chosen(meta)
    wide = (meta.shape[0], hidden)
    return jnp.broadcast_to(first, wide), jnp.broadcast_to(second, wide)


def parts_kernel(arr_ref, own_ref, sib_ref, x_ref, xsib_hbm, out_ref, xsib_ref, acc_ref, sem):
    fetch = pltpu.make_async_copy(xsib_hbm, xsib_ref, sem)
    fetch.start()
    w_refs = (own_ref, sib_ref, x_ref, xsib_ref)
    hidden = own_ref.shape[1]
    block = own_ref.shape[0] // 3
    half = block // 2
    mine = lax.axis_index("ep") & (GROUP - 1)
    first, second = picks(arr_ref[:, 2 * block :].astype(F32), hidden)

    def dense(q, r):
        if q < 2:
            return dot(arr_ref[:, :block], w_refs[r][q * block : (q + 1) * block, :], 1, 0)
        return dot(
            arr_ref[:, block : block + half], w_refs[r][2 * block : 2 * block + half, :], 1, 1
        ) + dot(arr_ref[:, block + half : 2 * block], w_refs[r][2 * block + half :, :], 1, 1)

    for q in range(3):
        p0 = jnp.zeros(first.shape, F32)
        p1 = p0
        for r in (0, 2, 1):
            part = dense(q, r)
            p0 = jnp.where(first == (mine ^ r), part, p0)
            p1 = jnp.where(second == (mine ^ r), part, p1)
        acc_ref[2 * q] = p0
        acc_ref[2 * q + 1] = p1
    fetch.wait()
    for q in range(3):
        part = dense(q, 3)
        p0 = jnp.where(first == (mine ^ 3), part, acc_ref[2 * q])
        p1 = jnp.where(second == (mine ^ 3), part, acc_ref[2 * q + 1])
        out_ref[:, q * hidden : (q + 1) * hidden] = p0.astype(BF)
        out_ref[:, (3 + q) * hidden : (4 + q) * hidden] = p1.astype(BF)


def act_kernel(part_ref, arr_ref, out_ref):
    share = part_ref.shape[1]
    hidden = part_ref.shape[2] // 6
    meta_at = arr_ref.shape[1] - LANES
    me = lax.axis_index("tp")

    def put(at, value):
        for copy in range(out_ref.shape[0]):
            out_ref[copy, :, at : at + value.shape[1]] = value

    meta = arr_ref[pl.ds(pl.multiple_of(me * share, share), share), meta_at:].astype(F32)
    first, second = chosen(meta)
    lane = iota((share, LANES), 1)
    extra = jnp.zeros((share, LANES), F32)
    for k, pick in enumerate((first, second)):
        weight = jnp.sum(jnp.where(lane == pick, meta, 0.0), axis=1, keepdims=True)
        total = []
        for q in range(3):
            at = slice((3 * k + q) * hidden, (3 * k + q + 1) * hidden)
            acc = part_ref[0, :, at].astype(F32)
            for d in range(1, part_ref.shape[0]):
                acc = acc + part_ref[d, :, at].astype(F32)
            total.append(acc)
        gate_pre, up_pre, grad_scaled = total
        sig = jax.nn.sigmoid(gate_pre)
        silu = gate_pre * sig
        hid = silu * up_pre
        gh = weight * grad_scaled
        at = 3 * k * hidden
        put(at, (weight * hid).astype(BF))
        put(at + hidden, (gh * up_pre * sig * (1.0 + gate_pre * (1.0 - sig))).astype(BF))
        put(at + 2 * hidden, (gh * silu).astype(BF))
        comb = jnp.sum(hid * grad_scaled, axis=1, keepdims=True)
        high = comb.astype(BF).astype(F32)
        extra = jnp.where(lane == 2 * k, high, jnp.where(lane == 2 * k + 1, comb - high, extra))
    put(6 * hidden, extra.astype(BF))


def masks(arr_ref, hidden, experts=ORDER):
    mine = lax.axis_index("ep") & (GROUP - 1)
    meta = arr_ref[:, arr_ref.shape[1] - LANES :].astype(F32)
    first, second = picks(meta, hidden)
    out = {}
    for r in experts:
        expert = mine ^ r
        out[r] = tuple(jnp.where(p == expert, 1.0, 0.0).astype(BF) for p in (first, second))
    return out


def spread(act_ref, mask, q, hidden):
    return (
        act_ref[:, q * hidden : (q + 1) * hidden] * mask[0]
        + act_ref[:, (3 + q) * hidden : (4 + q) * hidden] * mask[1]
    )


def back_kernel(act_ref, arr_ref, own_ref, sib_ref, x_ref, xsib_hbm, out_ref, xsib_ref, sem):
    hidden = own_ref.shape[1]
    block = own_ref.shape[0] // 3
    fetch = pltpu.make_async_copy(xsib_hbm.at[: 2 * block, :], xsib_ref, sem)
    fetch.start()
    w_refs = (own_ref, sib_ref, x_ref, xsib_ref)
    mask = masks(arr_ref, hidden)
    acc = jnp.zeros((act_ref.shape[0], block), F32)
    for r in ORDER:
        if r == 3:
            fetch.wait()
        for q in (1, 2):
            w = w_refs[r][(q - 1) * block : q * block, :]
            acc = acc + dot(spread(act_ref, mask[r], q, hidden), w, 1, 1)
    out_ref[:, :block] = acc.astype(BF)
    out_ref[:, block:] = act_ref[:, 6 * hidden :]


def inner_parts(act_ref, arr_ref, mask, hidden):
    rows = arr_ref[:, : (arr_ref.shape[1] - LANES) // 2]
    return [dot(rows, spread(act_ref, mask, q, hidden), 0, 0) for q in (1, 2)]


def outer_part(act_ref, arr_ref, mask, hidden):
    block = (arr_ref.shape[1] - LANES) // 2
    return dot(spread(act_ref, mask, 0, hidden), arr_ref[:, block : 2 * block], 0, 0)


def inner_kernel(act_ref, arr_ref, send_ref, pass_ref):
    hidden = send_ref.shape[1]
    block = send_ref.shape[0] // 2
    mask = masks(arr_ref, hidden, (2, 3))
    for r, ref in ((3, send_ref), (2, pass_ref)):
        gate, up = inner_parts(act_ref, arr_ref, mask[r], hidden)
        ref[:block, :] = gate.astype(BF)
        ref[block:, :] = up.astype(BF)


def outer_kernel(act_ref, arr_ref, send_ref, pass_ref):
    hidden = send_ref.shape[0]
    mask = masks(arr_ref, hidden, (2, 3))
    for r, ref in ((3, send_ref), (2, pass_ref)):
        ref[...] = outer_part(act_ref, arr_ref, mask[r], hidden).astype(BF)


def half_kernel(pass_ref, got_ref, out_ref):
    out_ref[...] = (pass_ref[...].astype(F32) + got_ref[...].astype(F32)).astype(BF)


def sibling_kernel(act_ref, arr_ref, out_ref):
    hidden = out_ref.shape[1]
    block = out_ref.shape[0] // 3
    half = block // 2
    mask = masks(arr_ref, hidden, (1,))[1]
    gate, up = inner_parts(act_ref, arr_ref, mask, hidden)
    down = outer_part(act_ref, arr_ref, mask, hidden).astype(BF)
    out_ref[:block, :] = gate.astype(BF)
    out_ref[block : 2 * block, :] = up.astype(BF)
    out_ref[2 * block : 2 * block + half, :] = down[:, :half]
    out_ref[2 * block + half :, :] = down[:, half:]


def base_kernel(act_ref, arr_ref, got_ref, inner_ref, outer_ref):
    hidden = inner_ref.shape[1]
    block = inner_ref.shape[0] // 2
    half = block // 2
    mask = masks(arr_ref, hidden, (0,))[0]
    gate, up = inner_parts(act_ref, arr_ref, mask, hidden)
    down = outer_part(act_ref, arr_ref, mask, hidden)
    inner_ref[:block, :] = (gate + got_ref[:block, :].astype(F32)).astype(BF)
    inner_ref[block:, :] = (up + got_ref[block : 2 * block, :].astype(F32)).astype(BF)
    left = down[:, :half] + got_ref[2 * block : 2 * block + half, :].astype(F32)
    right = down[:, half:] + got_ref[2 * block + half :, :].astype(F32)
    outer_ref[:, :half] = left.astype(BF)
    outer_ref[:, half:] = right.astype(BF)


def total_kernel(base_ref, last_ref, *out_refs):
    rows = out_refs[0].shape[0]
    for i, out_ref in enumerate(out_refs):
        at = slice(i * rows, (i + 1) * rows)
        out_ref[...] = base_ref[at, :].astype(F32) + last_ref[at, :].astype(F32)


def final_kernel(ret_ref, exp_ref, tok_ref, comb_ref):
    block = tok_ref.shape[1]
    experts = exp_ref[...]
    place = placement(experts, ret_ref.shape[0] // CAP)
    tok_ref[...] = dot(place, ret_ref[:, :block], 0, 0).astype(BF)
    extra = dot(ret_ref[:, block:], place, 0, 0)
    low = extra[0:1, :] + extra[1:2, :]
    high = extra[2:3, :] + extra[3:4, :]
    rising = experts[0:1, :] < experts[1:2, :]
    comb_ref[0:1, :] = jnp.where(rising, low, high)
    comb_ref[1:2, :] = jnp.where(rising, high, low)


def body(tokens, cotangent, experts, combine, w_gate, w_up, w_down):
    peers = lax.axis_size("ep")
    widths = lax.axis_size("tp")
    toks, block = tokens.shape
    hidden = w_gate.shape[2]
    n_groups = peers // GROUP
    slots = n_groups * CAP
    share = slots // widths
    groups = exchange_groups(peers)
    half = block // 2

    sources = (tokens, cotangent, experts.T, combine.T)
    payload = call(
        send_kernel,
        shape((slots, 2 * block + LANES), BF),
        *(pltpu.with_memory_space_constraint(a, pltpu.HBM) for a in sources),
        in_specs=[pl.BlockSpec(memory_space=pltpu.HBM)] * 4,
        out_specs=pl.BlockSpec(memory_space=pltpu.HBM),
        scratch_shapes=[pltpu.VMEM(a.shape, a.dtype) for a in sources]
        + [pltpu.VMEM((slots, 2 * block + LANES), BF), pltpu.SemaphoreType.DMA((6,))],
    )
    arrived = lax.all_to_all(
        payload.reshape(n_groups, CAP, -1),
        "ep",
        split_axis=0,
        concat_axis=0,
        tiled=True,
        axis_index_groups=groups,
    ).reshape(slots, -1)
    arrived = pltpu.with_memory_space_constraint(arrived, pltpu.VMEM)
    own = jnp.concatenate([w_gate[0], w_up[0], w_down[0][:, :half], w_down[0][:, half:]], axis=0)
    other = lax.ppermute(own, "ep", partner(peers, 2))
    sibling = lax.ppermute(own, "ep", partner(peers, 1))
    across = lax.ppermute(other, "ep", partner(peers, 1))
    w_all = tuple(
        pltpu.with_memory_space_constraint(w, space)
        for w, space in zip((own, sibling, other, across), (pltpu.VMEM,) * 3 + (pltpu.HBM,))
    )
    parts = call(
        parts_kernel,
        shape((slots, 6 * hidden), BF),
        arrived,
        *w_all,
        in_specs=[pl.BlockSpec(memory_space=pltpu.HBM if i == 4 else pltpu.VMEM) for i in range(5)],
        scratch_shapes=[
            pltpu.VMEM((3 * block, hidden), BF),
            pltpu.VMEM((6, slots, hidden), F32),
            pltpu.SemaphoreType.DMA,
        ],
    )
    pieces = lax.all_to_all(
        parts.reshape(widths, share, -1), "tp", split_axis=0, concat_axis=0, tiled=True
    )
    acts = call(act_kernel, shape((widths, share, 6 * hidden + LANES), BF), pieces, arrived)
    acts = lax.all_to_all(acts, "tp", split_axis=0, concat_axis=0, tiled=True)
    acts = acts.reshape(slots, -1)
    acts = pltpu.with_memory_space_constraint(acts, pltpu.VMEM)
    back = call(
        back_kernel,
        shape((slots, block + LANES), BF),
        acts,
        arrived,
        *w_all,
        in_specs=[pl.BlockSpec(memory_space=pltpu.HBM if i == 5 else pltpu.VMEM) for i in range(6)],
        scratch_shapes=[pltpu.VMEM((2 * block, hidden), BF), pltpu.SemaphoreType.DMA],
    )
    returned = lax.all_to_all(
        back.reshape(n_groups, CAP, -1),
        "ep",
        split_axis=0,
        concat_axis=0,
        tiled=True,
        axis_index_groups=groups,
    ).reshape(slots, -1)
    pairs = []
    for kernel, inputs, dims in (
        (inner_kernel, (acts, arrived), (2 * block, hidden)),
        (outer_kernel, (acts, arrived), (hidden, block)),
    ):
        send, through = call(kernel, (shape(dims, BF), shape(dims, BF)), *inputs)
        got = lax.ppermute(send, "ep", partner(peers, 1))
        pair = call(half_kernel, shape(dims, BF), through, got)
        pairs.append(lax.ppermute(pair, "ep", partner(peers, 2)))
    send = call(sibling_kernel, shape((3 * block, hidden), BF), acts, arrived)
    got = lax.ppermute(send, "ep", partner(peers, 1))
    base = call(
        base_kernel,
        (shape((2 * block, hidden), BF), shape((hidden, block), BF)),
        acts,
        arrived,
        got,
    )
    gate_grad, up_grad = call(total_kernel, (shape((block, hidden), F32),) * 2, base[0], pairs[0])
    (down_grad,) = call(total_kernel, (shape((hidden, block), F32),), base[1], pairs[1])
    grad_tokens, comb = call(
        final_kernel, (shape((toks, block), BF), shape((2, toks), F32)), returned, experts.T
    )
    return (grad_tokens, comb.T, gate_grad[None], up_grad[None], down_grad[None])


def solution(mesh):
    return jax.shard_map(
        body,
        mesh=mesh,
        in_specs=(
            P("ep", "tp"),
            P("ep", "tp"),
            P("ep", None),
            P("ep", None),
            P("ep", "tp", None),
            P("ep", "tp", None),
            P("ep", None, "tp"),
        ),
        out_specs=(
            P("ep", "tp"),
            P("ep", None),
            P("ep", "tp", None),
            P("ep", "tp", None),
            P("ep", None, "tp"),
        ),
        check_vma=False,
    )
```

```python
import jax
import jax.numpy as jnp
from jax import lax
from jax.experimental import pallas as pl
from jax.experimental.pallas import tpu as pltpu
from jax.sharding import PartitionSpec as P

BF = jnp.bfloat16
F32 = jnp.float32
I32 = jnp.int32
GROUP = 4
CAP = 8
LANES = 128
ORDER = (0, 2, 1, 3)


def exchange_groups(peers):
    planes = peers // 8
    groups = []
    for low in (0, 1):
        for core in (0, 1):
            groups.append(
                [
                    z * 8 + x * 2 + core
                    for near in range(planes // 4)
                    for z in (near + planes // 4 * q for q in (0, 2, 1, 3))
                    for x in (low, 3 - low)
                ]
            )
    return groups


def partner(peers, bit):
    return [(i, i ^ bit) for i in range(peers)]


def dot(a, b, ca, cb):
    return lax.dot_general(a, b, (((ca,), (cb,)), ((), ())), preferred_element_type=F32)


def iota(shape, dim):
    return lax.broadcasted_iota(I32, shape, dim)


def call(kernel, outs, *args, **kwargs):
    return pl.pallas_call(
        kernel,
        out_shape=outs,
        compiler_params=pltpu.CompilerParams(vmem_limit_bytes=20 * 1024 * 1024),
        **kwargs,
    )(*args)


def shape(dims, dtype):
    return jax.ShapeDtypeStruct(dims, dtype)


def placement(experts, n_groups):
    toks = experts.shape[1]
    group = lax.shift_right_logical(experts[0:1, :], 2)
    plane = lax.shift_right_logical(group, 1)
    planes = n_groups // 2
    quarter = plane // (planes // 4)
    middle = (quarter == 1) | (quarter == 2)
    plane = plane % (planes // 4) * 4 + jnp.where(middle, 3 - quarter, quarter)
    group = 2 * plane + (group & 1)
    member = iota((n_groups, toks), 0) == group
    onehot = jnp.where(member, 1.0, 0.0)
    earlier = jnp.where(iota((toks, toks), 0) < iota((toks, toks), 1), 1.0, 0.0).astype(BF)
    cum = dot(onehot.astype(BF), earlier, 1, 0)
    pos = jnp.sum(onehot * cum, axis=0, keepdims=True).astype(I32)
    slot = group * CAP + pos
    return jnp.where(iota((n_groups * CAP, toks), 0) == slot, 1.0, 0.0).astype(BF)


def send_kernel(
    tok_hbm, cot_hbm, exp_hbm, comb_hbm, out_hbm, tok_ref, cot_ref, exp_ref, comb_ref, out_ref, sems
):
    copies = [
        pltpu.make_async_copy(src, dst, sems.at[i])
        for i, (src, dst) in enumerate(
            ((exp_hbm, exp_ref), (tok_hbm, tok_ref), (cot_hbm, cot_ref), (comb_hbm, comb_ref))
        )
    ]
    for copy in copies:
        copy.start()
    toks, block = tok_ref.shape
    n_groups = out_ref.shape[0] // CAP
    copies[0].wait()
    experts = exp_ref[...]
    place = placement(experts, n_groups)
    local = experts & (GROUP - 1)
    row = iota((LANES, toks), 0)

    def written(first, last, i):
        copy = pltpu.make_async_copy(
            out_ref.at[:, first:last], out_hbm.at[:, first:last], sems.at[len(copies) + i]
        )
        copy.start()
        return copy

    copies[1].wait()
    out_ref[:, :block] = dot(place, tok_ref[...], 1, 0).astype(BF)
    rows_out = written(0, block, 0)
    copies[2].wait()
    copies[3].wait()
    weight = comb_ref[...].astype(BF).astype(F32)
    meta = jnp.where(row == local[0:1, :], weight[0:1, :], 0.0) + jnp.where(
        row == local[1:2, :], weight[1:2, :], 0.0
    )
    out_ref[:, block : 2 * block] = dot(place, cot_ref[...], 1, 0).astype(BF)
    out_ref[:, 2 * block :] = dot(place, meta.astype(BF), 1, 1).astype(BF)
    rest_out = written(block, 2 * block + LANES, 1)
    rows_out.wait()
    rest_out.wait()


def chosen(meta):
    lane = iota(meta.shape, 1)
    used = meta > 0
    first = jnp.min(jnp.where(used, lane, 99), axis=1, keepdims=True)
    second = jnp.max(jnp.where(used, lane, -1), axis=1, keepdims=True)
    return first, second


def picks(meta, hidden):
    first, second = chosen(meta)
    wide = (meta.shape[0], hidden)
    return jnp.broadcast_to(first, wide), jnp.broadcast_to(second, wide)


def parts_kernel(arr_ref, own_ref, sib_ref, x_ref, xsib_hbm, out_ref, xsib_ref, acc_ref, sem):
    fetch = pltpu.make_async_copy(xsib_hbm, xsib_ref, sem)
    fetch.start()
    w_refs = (own_ref, sib_ref, x_ref, xsib_ref)
    hidden = own_ref.shape[1]
    block = own_ref.shape[0] // 3
    half = block // 2
    mine = lax.axis_index("ep") & (GROUP - 1)
    first, second = picks(arr_ref[:, 2 * block :].astype(F32), hidden)

    def dense(q, r):
        if q < 2:
            return dot(arr_ref[:, :block], w_refs[r][q * block : (q + 1) * block, :], 1, 0)
        return dot(
            arr_ref[:, block : block + half], w_refs[r][2 * block : 2 * block + half, :], 1, 1
        ) + dot(arr_ref[:, block + half : 2 * block], w_refs[r][2 * block + half :, :], 1, 1)

    for q in range(3):
        p0 = jnp.zeros(first.shape, F32)
        p1 = p0
        for r in (0, 2, 1):
            part = dense(q, r)
            p0 = jnp.where(first == (mine ^ r), part, p0)
            p1 = jnp.where(second == (mine ^ r), part, p1)
        acc_ref[2 * q] = p0
        acc_ref[2 * q + 1] = p1
    fetch.wait()
    for q in range(3):
        part = dense(q, 3)
        p0 = jnp.where(first == (mine ^ 3), part, acc_ref[2 * q])
        p1 = jnp.where(second == (mine ^ 3), part, acc_ref[2 * q + 1])
        out_ref[:, q * hidden : (q + 1) * hidden] = p0.astype(BF)
        out_ref[:, (3 + q) * hidden : (4 + q) * hidden] = p1.astype(BF)


def act_kernel(part_ref, arr_ref, out_ref):
    share = part_ref.shape[1]
    hidden = part_ref.shape[2] // 6
    meta_at = arr_ref.shape[1] - LANES
    me = lax.axis_index("tp")
    meta = arr_ref[pl.ds(pl.multiple_of(me * share, share), share), meta_at:].astype(F32)
    first, second = chosen(meta)
    lane = iota((share, LANES), 1)
    extra = jnp.zeros((share, LANES), F32)
    for k, pick in enumerate((first, second)):
        weight = jnp.sum(jnp.where(lane == pick, meta, 0.0), axis=1, keepdims=True)
        total = []
        for q in range(3):
            at = slice((3 * k + q) * hidden, (3 * k + q + 1) * hidden)
            acc = part_ref[0, :, at].astype(F32)
            for d in range(1, part_ref.shape[0]):
                acc = acc + part_ref[d, :, at].astype(F32)
            total.append(acc)
        gate_pre, up_pre, grad_scaled = total
        sig = jax.nn.sigmoid(gate_pre)
        silu = gate_pre * sig
        hid = silu * up_pre
        gh = weight * grad_scaled
        at = 3 * k * hidden
        out_ref[:, at : at + hidden] = (weight * hid).astype(BF)
        out_ref[:, at + hidden : at + 2 * hidden] = (
            gh * up_pre * sig * (1.0 + gate_pre * (1.0 - sig))
        ).astype(BF)
        out_ref[:, at + 2 * hidden : at + 3 * hidden] = (gh * silu).astype(BF)
        comb = jnp.sum(hid * grad_scaled, axis=1, keepdims=True)
        high = comb.astype(BF).astype(F32)
        extra = jnp.where(lane == 2 * k, high, jnp.where(lane == 2 * k + 1, comb - high, extra))
    out_ref[:, 6 * hidden :] = extra.astype(BF)


def masks(arr_ref, hidden, experts=ORDER):
    mine = lax.axis_index("ep") & (GROUP - 1)
    meta = arr_ref[:, arr_ref.shape[1] - LANES :].astype(F32)
    first, second = picks(meta, hidden)
    out = {}
    for r in experts:
        expert = mine ^ r
        out[r] = tuple(jnp.where(p == expert, 1.0, 0.0).astype(BF) for p in (first, second))
    return out


def spread(act_ref, mask, q, hidden):
    return (
        act_ref[:, q * hidden : (q + 1) * hidden] * mask[0]
        + act_ref[:, (3 + q) * hidden : (4 + q) * hidden] * mask[1]
    )


def back_kernel(act_ref, arr_ref, own_ref, sib_ref, x_ref, xsib_hbm, out_ref, xsib_ref, sem):
    hidden = own_ref.shape[1]
    block = own_ref.shape[0] // 3
    fetch = pltpu.make_async_copy(xsib_hbm.at[: 2 * block, :], xsib_ref, sem)
    fetch.start()
    w_refs = (own_ref, sib_ref, x_ref, xsib_ref)
    mask = masks(arr_ref, hidden)
    acc = jnp.zeros((act_ref.shape[0], block), F32)
    for r in ORDER:
        if r == 3:
            fetch.wait()
        for q in (1, 2):
            w = w_refs[r][(q - 1) * block : q * block, :]
            acc = acc + dot(spread(act_ref, mask[r], q, hidden), w, 1, 1)
    out_ref[:, :block] = acc.astype(BF)
    out_ref[:, block:] = act_ref[:, 6 * hidden :]


def inner_parts(act_ref, arr_ref, mask, hidden):
    rows = arr_ref[:, : (arr_ref.shape[1] - LANES) // 2]
    return [dot(rows, spread(act_ref, mask, q, hidden), 0, 0) for q in (1, 2)]


def outer_part(act_ref, arr_ref, mask, hidden):
    block = (arr_ref.shape[1] - LANES) // 2
    return dot(spread(act_ref, mask, 0, hidden), arr_ref[:, block : 2 * block], 0, 0)


def inner_kernel(act_ref, arr_ref, send_ref, pass_ref):
    hidden = send_ref.shape[1]
    block = send_ref.shape[0] // 2
    mask = masks(arr_ref, hidden, (2, 3))
    for r, ref in ((3, send_ref), (2, pass_ref)):
        gate, up = inner_parts(act_ref, arr_ref, mask[r], hidden)
        ref[:block, :] = gate.astype(BF)
        ref[block:, :] = up.astype(BF)


def outer_kernel(act_ref, arr_ref, send_ref, pass_ref):
    hidden = send_ref.shape[0]
    mask = masks(arr_ref, hidden, (2, 3))
    for r, ref in ((3, send_ref), (2, pass_ref)):
        ref[...] = outer_part(act_ref, arr_ref, mask[r], hidden).astype(BF)


def half_kernel(pass_ref, got_ref, out_ref):
    out_ref[...] = (pass_ref[...].astype(F32) + got_ref[...].astype(F32)).astype(BF)


def sibling_kernel(act_ref, arr_ref, out_ref):
    hidden = out_ref.shape[1]
    block = out_ref.shape[0] // 3
    half = block // 2
    mask = masks(arr_ref, hidden, (1,))[1]
    gate, up = inner_parts(act_ref, arr_ref, mask, hidden)
    down = outer_part(act_ref, arr_ref, mask, hidden).astype(BF)
    out_ref[:block, :] = gate.astype(BF)
    out_ref[block : 2 * block, :] = up.astype(BF)
    out_ref[2 * block : 2 * block + half, :] = down[:, :half]
    out_ref[2 * block + half :, :] = down[:, half:]


def base_kernel(act_ref, arr_ref, got_ref, inner_ref, outer_ref):
    hidden = inner_ref.shape[1]
    block = inner_ref.shape[0] // 2
    half = block // 2
    mask = masks(arr_ref, hidden, (0,))[0]
    gate, up = inner_parts(act_ref, arr_ref, mask, hidden)
    down = outer_part(act_ref, arr_ref, mask, hidden)
    inner_ref[:block, :] = (gate + got_ref[:block, :].astype(F32)).astype(BF)
    inner_ref[block:, :] = (up + got_ref[block : 2 * block, :].astype(F32)).astype(BF)
    left = down[:, :half] + got_ref[2 * block : 2 * block + half, :].astype(F32)
    right = down[:, half:] + got_ref[2 * block + half :, :].astype(F32)
    outer_ref[:, :half] = left.astype(BF)
    outer_ref[:, half:] = right.astype(BF)


def total_kernel(base_ref, last_ref, *out_refs):
    rows = out_refs[0].shape[0]
    for i, out_ref in enumerate(out_refs):
        at = slice(i * rows, (i + 1) * rows)
        out_ref[...] = base_ref[at, :].astype(F32) + last_ref[at, :].astype(F32)


def final_kernel(ret_ref, exp_ref, tok_ref, comb_ref):
    block = tok_ref.shape[1]
    experts = exp_ref[...]
    place = placement(experts, ret_ref.shape[0] // CAP)
    tok_ref[...] = dot(place, ret_ref[:, :block], 0, 0).astype(BF)
    extra = dot(ret_ref[:, block:], place, 0, 0)
    low = extra[0:1, :] + extra[1:2, :]
    high = extra[2:3, :] + extra[3:4, :]
    rising = experts[0:1, :] < experts[1:2, :]
    comb_ref[0:1, :] = jnp.where(rising, low, high)
    comb_ref[1:2, :] = jnp.where(rising, high, low)


def body(tokens, cotangent, experts, combine, w_gate, w_up, w_down):
    peers = lax.axis_size("ep")
    widths = lax.axis_size("tp")
    toks, block = tokens.shape
    hidden = w_gate.shape[2]
    n_groups = peers // GROUP
    slots = n_groups * CAP
    share = slots // widths
    groups = exchange_groups(peers)
    half = block // 2

    sources = (tokens, cotangent, experts.T, combine.T)
    payload = call(
        send_kernel,
        shape((slots, 2 * block + LANES), BF),
        *(pltpu.with_memory_space_constraint(a, pltpu.HBM) for a in sources),
        in_specs=[pl.BlockSpec(memory_space=pltpu.HBM)] * 4,
        out_specs=pl.BlockSpec(memory_space=pltpu.HBM),
        scratch_shapes=[pltpu.VMEM(a.shape, a.dtype) for a in sources]
        + [pltpu.VMEM((slots, 2 * block + LANES), BF), pltpu.SemaphoreType.DMA((6,))],
    )
    arrived = lax.all_to_all(
        payload.reshape(n_groups, CAP, -1),
        "ep",
        split_axis=0,
        concat_axis=0,
        tiled=True,
        axis_index_groups=groups,
    ).reshape(slots, -1)
    arrived = pltpu.with_memory_space_constraint(arrived, pltpu.VMEM)
    own = jnp.concatenate([w_gate[0], w_up[0], w_down[0][:, :half], w_down[0][:, half:]], axis=0)
    other = lax.ppermute(own, "ep", partner(peers, 2))
    sibling = lax.ppermute(own, "ep", partner(peers, 1))
    across = lax.ppermute(other, "ep", partner(peers, 1))
    w_all = tuple(
        pltpu.with_memory_space_constraint(w, space)
        for w, space in zip((own, sibling, other, across), (pltpu.VMEM,) * 3 + (pltpu.HBM,))
    )
    parts = call(
        parts_kernel,
        shape((slots, 6 * hidden), BF),
        arrived,
        *w_all,
        in_specs=[pl.BlockSpec(memory_space=pltpu.HBM if i == 4 else pltpu.VMEM) for i in range(5)],
        scratch_shapes=[
            pltpu.VMEM((3 * block, hidden), BF),
            pltpu.VMEM((6, slots, hidden), F32),
            pltpu.SemaphoreType.DMA,
        ],
    )
    pieces = lax.all_to_all(
        parts.reshape(widths, share, -1), "tp", split_axis=0, concat_axis=0, tiled=True
    )
    acts = call(act_kernel, shape((share, 6 * hidden + LANES), BF), pieces, arrived)
    acts = lax.all_gather(acts, "tp", axis=0, tiled=True)
    acts = pltpu.with_memory_space_constraint(acts, pltpu.VMEM)
    back = call(
        back_kernel,
        shape((slots, block + LANES), BF),
        acts,
        arrived,
        *w_all,
        in_specs=[pl.BlockSpec(memory_space=pltpu.HBM if i == 5 else pltpu.VMEM) for i in range(6)],
        scratch_shapes=[pltpu.VMEM((2 * block, hidden), BF), pltpu.SemaphoreType.DMA],
    )
    returned = lax.all_to_all(
        back.reshape(n_groups, CAP, -1),
        "ep",
        split_axis=0,
        concat_axis=0,
        tiled=True,
        axis_index_groups=groups,
    ).reshape(slots, -1)
    pairs = []
    for kernel, inputs, dims in (
        (inner_kernel, (acts, arrived), (2 * block, hidden)),
        (outer_kernel, (acts, arrived), (hidden, block)),
    ):
        send, through = call(kernel, (shape(dims, BF), shape(dims, BF)), *inputs)
        got = lax.ppermute(send, "ep", partner(peers, 1))
        pair = call(half_kernel, shape(dims, BF), through, got)
        pairs.append(lax.ppermute(pair, "ep", partner(peers, 2)))
    send = call(sibling_kernel, shape((3 * block, hidden), BF), acts, arrived)
    got = lax.ppermute(send, "ep", partner(peers, 1))
    base = call(
        base_kernel,
        (shape((2 * block, hidden), BF), shape((hidden, block), BF)),
        acts,
        arrived,
        got,
    )
    gate_grad, up_grad = call(total_kernel, (shape((block, hidden), F32),) * 2, base[0], pairs[0])
    (down_grad,) = call(total_kernel, (shape((hidden, block), F32),), base[1], pairs[1])
    grad_tokens, comb = call(
        final_kernel, (shape((toks, block), BF), shape((2, toks), F32)), returned, experts.T
    )
    return (grad_tokens, comb.T, gate_grad[None], up_grad[None], down_grad[None])


def solution(mesh):
    return jax.shard_map(
        body,
        mesh=mesh,
        in_specs=(
            P("ep", "tp"),
            P("ep", "tp"),
            P("ep", None),
            P("ep", None),
            P("ep", "tp", None),
            P("ep", "tp", None),
            P("ep", None, "tp"),
        ),
        out_specs=(
            P("ep", "tp"),
            P("ep", None),
            P("ep", "tp", None),
            P("ep", "tp", None),
            P("ep", None, "tp"),
        ),
        check_vma=False,
    )
```
